32 devices in a mesh: sp: 8 (over z, y), tp: 4 (over x, core).
Axes of the slice: x: 2, y: 2, z: 4, core: 2. Of those that a mesh axis runs over, the one named last changes fastest.
Arguments:
- resid: bfloat16 [2048, 2048], P(('sp', 'tp')), may hold values from -0.21875 to 0.21875
- query_a: bfloat16 [2048, 1024], P('sp', 'tp'), may hold values from -6 to 6
- key_a: bfloat16 [2048, 256], P('sp', 'tp'), may hold values from -6 to 6
- value_a: bfloat16 [2048, 256], P('sp', 'tp'), may hold values from -6 to 6
- query_b: bfloat16 [2048, 1024], P('sp', 'tp'), may hold values from -6 to 6
- key_b: bfloat16 [2048, 512], P('sp', 'tp'), may hold values from -6 to 6
- value_b: bfloat16 [2048, 512], P('sp', 'tp'), may hold values from -6 to 6
- gain_qa: float32 [64], replicated, may hold values from 0.1 to 8
- gain_ka: float32 [64], replicated, may hold values from 0.1 to 8
- gain_qb: float32 [128], replicated, may hold values from 0.1 to 8
- gain_kb: float32 [128], replicated, may hold values from 0.1 to 8
- w_out_a: bfloat16 [1024, 2048], P('tp'), may hold values from -0.125 to 0.125
- w_out_b: bfloat16 [1024, 2048], P('tp'), may hold values from -0.125 to 0.125
- norm_gain: float32 [2048], replicated, may hold values from 0.1 to 1.9
- w_up: bfloat16 [2048, 8192], P('sp', 'tp'), may hold values from -0.125 to 0.125
- w_down: bfloat16 [8192, 2048], P('tp', 'sp'), may hold values from -0.0625 to 0.0625
Outputs:
- result: bfloat16 [2048, 2048], P(('sp', 'tp'))
The draws below stay inside these ranges and needn't reach their ends.
All inputs are finite; a program needn't handle non-finite values.
Results may differ from the reference program's by a relative error of at most 0.02.
The reference program's roundings to bfloat16 on the way count: a program that leaves them out, or rounds other values in their place, can miss the bound.
Values may be sent and summed in bfloat16 or wider, within the bound.
No kernel may reach another device: no remote copies, remote signals or barrier semaphores. Data moves between devices by JAX's collectives and lax.ppermute only.
A program may use at most 128 MiB of HBM per device.

```python
import math
import jax
import jax.numpy as jnp
from jax import lax

D = 2048
FF = 8192
HD_A = 64
HD_B = 128
HEADS_A = 16
HEADS_B = 8
KV_A = 4
KV_B = 4
GRID_W = 64
TOKENS = 2048
ATT_W = 2048


def pair_draw(key, heads, kv_heads, width, salt):
    base = jax.random.fold_in(key, salt)
    keys = jnp.clip(jax.random.normal(jax.random.fold_in(base, 1), (TOKENS, kv_heads * width), jnp.float32), -6.0, 6.0)
    queries = jnp.clip(jax.random.normal(jax.random.fold_in(base, 2), (TOKENS, heads * width), jnp.float32), -6.0, 6.0)
    return (queries.astype(jnp.bfloat16), keys.astype(jnp.bfloat16))


def gain_draw(key, width, salt):
    inner = jax.random.fold_in(key, salt)
    return jnp.clip(1.0 + 0.18 * jax.random.normal(inner, (width,), jnp.float32), 0.1, 1.9)


def draw_query_a(key, part):
    return pair_draw(key, HEADS_A, KV_A, HD_A, 101)[0]


def draw_key_a(key, part):
    return pair_draw(key, HEADS_A, KV_A, HD_A, 101)[1]


def draw_query_b(key, part):
    return pair_draw(key, HEADS_B, KV_B, HD_B, 202)[0]


def draw_key_b(key, part):
    return pair_draw(key, HEADS_B, KV_B, HD_B, 202)[1]


def draw_gain_qa(key, part):
    return gain_draw(key, HD_A, 31)


def draw_gain_ka(key, part):
    return gain_draw(key, HD_A, 32)


def draw_gain_qb(key, part):
    return gain_draw(key, HD_B, 33)


def draw_gain_kb(key, part):
    return gain_draw(key, HD_B, 34)


def shard_levels(own_key, extent, pieces, least, high):
    factor_of = 1.0
    for dim, blocks in pieces:
        heights = jax.random.uniform(jax.random.fold_in(jax.random.fold_in(own_key, 6), dim), (blocks,), jnp.float32, least / len(pieces), high / len(pieces))
        factor_of = factor_of * jnp.repeat(jnp.exp(heights), extent[dim] // blocks).reshape((-1,) + (1,) * (len(extent) - 1 - dim))
    return factor_of


def normal_values(rng, extent, scale, reach, cuts=(), kind=jnp.bfloat16):
    entries = jax.random.normal(rng, extent, jnp.float32) * scale
    if len(cuts) > 0:
        entries = shard_levels(rng, extent, cuts, -0.22, 0.18) * entries
    return jnp.clip(entries, min=-reach, max=reach).astype(kind)


def setup_inputs(seed: int = 0) -> dict:
    key_of = jax.random.split(jax.random.key(seed), 17)
    return {
        "resid": normal_values(key_of[0], (TOKENS, D), 0.015, 0.21875, ((0, 32),)),
        "query_a": draw_query_a(jax.random.fold_in(key_of[16], 71), 0),
        "key_a": draw_key_a(jax.random.fold_in(key_of[16], 71), 0),
        "value_a": normal_values(key_of[3], (TOKENS, KV_A * HD_A), 1.0, 6.0, ((0, 8), (1, 4))),
        "query_b": draw_query_b(jax.random.fold_in(key_of[16], 71), 0),
        "key_b": draw_key_b(jax.random.fold_in(key_of[16], 71), 0),
        "value_b": normal_values(key_of[6], (TOKENS, KV_B * HD_B), 1.0, 6.0, ((0, 8), (1, 4))),
        "gain_qa": draw_gain_qa(jax.random.fold_in(key_of[16], 71), 0),
        "gain_ka": draw_gain_ka(jax.random.fold_in(key_of[16], 71), 0),
        "gain_qb": draw_gain_qb(jax.random.fold_in(key_of[16], 71), 0),
        "gain_kb": draw_gain_kb(jax.random.fold_in(key_of[16], 71), 0),
        "w_out_a": normal_values(key_of[11], (HEADS_A * HD_A, D), ATT_W ** -0.5, 0.125, ((0, 4),)),
        "w_out_b": normal_values(key_of[12], (HEADS_B * HD_B, D), ATT_W ** -0.5, 0.125, ((0, 4),)),
        "norm_gain": jnp.clip(1.0 + 0.18 * jax.random.normal(key_of[13], (D,), jnp.float32), 0.1, 1.9),
        "w_up": normal_values(key_of[14], (D, FF), D ** -0.5, 0.125, ((0, 8), (1, 4))),
        "w_down": normal_values(key_of[15], (FF, D), FF ** -0.5, 0.0625, ((0, 4), (1, 8))),
    }


EPS = 1e-06

def tables(count, width):
    pos = jnp.arange(count, dtype=jnp.int32)
    grid_rows = (pos // GRID_W).astype(jnp.float32)
    grid_cols = (pos % GRID_W).astype(jnp.float32)
    quarter = width // 4
    freqs = 10000.0 ** (-(2.0 * jnp.arange(quarter, dtype=jnp.float32)) / (width // 2))
    ang_r = grid_rows[:, None] * freqs
    ang_c = grid_cols[:, None] * freqs
    angles = jnp.concatenate([ang_r, ang_r, ang_c, ang_c], axis=-1)
    return (jnp.cos(angles), jnp.sin(angles))

def norm_rope(values, gain, width):
    count = values.shape[0]
    flat = values.astype(jnp.float32).reshape(count, -1, width)
    flat = flat * lax.rsqrt(lax.optimization_barrier(jnp.mean(flat * flat, axis=-1, keepdims=True)) + EPS) * gain.astype(jnp.float32)
    cosine, sine = tables(count, width)
    one, two, three, four = jnp.split(flat, 4, axis=-1)
    turned = jnp.concatenate([-two, one, -four, three], axis=-1)
    return (flat * cosine[:, None, :] + turned * sine[:, None, :]).astype(jnp.bfloat16)

def attend(queries, keys, values, width):
    count, heads = (queries.shape[0], queries.shape[1])
    kv_heads = keys.shape[1]
    groups = heads // kv_heads
    block = math.gcd(count, 256)
    keys32 = keys.astype(jnp.float32)
    vals32 = values.astype(jnp.float32).reshape(count, kv_heads, width)
    blocks = queries.reshape(count // block, block, kv_heads, groups, width)
    scale = width ** (-0.5)

    def one_block(qblock):
        scores = jnp.einsum('rkgd,pkd->kgrp', qblock.astype(jnp.float32), keys32) * scale
        top = lax.optimization_barrier(jnp.max(scores, axis=-1, keepdims=True))
        expo = jnp.exp(scores - top)
        probs = expo.astype(jnp.bfloat16).astype(jnp.float32)
        summed = jnp.einsum('kgrp,pkd->kgrd', probs, vals32)
        outputs = summed / lax.optimization_barrier(jnp.sum(expo, axis=-1))[..., None]
        return jnp.transpose(outputs, (2, 0, 1, 3)).reshape(block, heads * width).astype(jnp.bfloat16)
    return lax.map(one_block, blocks).reshape(count, heads * width)

def reference(resid, query_a, key_a, value_a, query_b, key_b, value_b, gain_qa, gain_ka, gain_qb, gain_kb, w_out_a, w_out_b, norm_gain, w_up, w_down):
    width_a = gain_qa.shape[0]
    width_b = gain_qb.shape[0]
    attn_a = attend(norm_rope(query_a, gain_qa, width_a), norm_rope(key_a, gain_ka, width_a), value_a, width_a)
    attn_b = attend(norm_rope(query_b, gain_qb, width_b), norm_rope(key_b, gain_kb, width_b), value_b, width_b)
    proj = jnp.dot(attn_a, w_out_a, preferred_element_type=jnp.float32) + jnp.dot(attn_b, w_out_b, preferred_element_type=jnp.float32)
    mid = (resid.astype(jnp.float32) + proj).astype(jnp.bfloat16)
    midf = mid.astype(jnp.float32)
    normed = (midf * lax.rsqrt(lax.optimization_barrier(jnp.mean(midf * midf, axis=-1, keepdims=True)) + EPS) * norm_gain).astype(jnp.bfloat16)
    hidden = jnp.square(jax.nn.relu(jnp.dot(normed, w_up, preferred_element_type=jnp.float32))).astype(jnp.bfloat16)
    return (midf + jnp.dot(hidden, w_down, preferred_element_type=jnp.float32)).astype(jnp.bfloat16)
```

```python
import math

import jax
import jax.numpy as jnp
from jax import lax
from jax.sharding import PartitionSpec as P

GRID_W = 64
EPS = 1e-06


def norm_rope(values, gain, places):
    width = gain.shape[0]
    count = values.shape[0]
    flat = values.astype(jnp.float32).reshape(count, -1, width)
    flat = flat * lax.rsqrt(jnp.mean(flat * flat, axis=-1, keepdims=True) + EPS) * gain
    grid_rows = (places // GRID_W).astype(jnp.float32)
    grid_cols = (places % GRID_W).astype(jnp.float32)
    quarter = width // 4
    freqs = 10000.0 ** (-(2.0 * jnp.arange(quarter, dtype=jnp.float32)) / (width // 2))
    ang_r = grid_rows[:, None] * freqs
    ang_c = grid_cols[:, None] * freqs
    angles = jnp.concatenate([ang_r, ang_r, ang_c, ang_c], axis=-1)
    one, two, three, four = jnp.split(flat, 4, axis=-1)
    turned = jnp.concatenate([-two, one, -four, three], axis=-1)
    return (flat * jnp.cos(angles)[:, None, :] + turned * jnp.sin(angles)[:, None, :]).astype(
        jnp.bfloat16
    )


def attend(queries, keys, values, scale):
    scores = (
        jnp.einsum("rkgd,pkd->kgrp", queries, keys, preferred_element_type=jnp.float32) * scale
    )
    top = jnp.max(scores, axis=-1, keepdims=True)
    expo = jnp.exp(scores - top)
    total = jnp.sum(expo, axis=-1)
    accum = jnp.einsum(
        "kgrp,pkd->kgrd",
        expo.astype(jnp.bfloat16),
        values,
        preferred_element_type=jnp.float32,
    )
    outputs = accum / total[..., None]
    return jnp.transpose(outputs, (2, 0, 1, 3)).reshape(queries.shape[0], -1).astype(jnp.bfloat16)


def make_local(sp, tp):
    low, core = 2, 2
    high, wide = sp // low, tp // core
    assert high * low == sp and wide * core == tp and wide == 2

    def over_high(value, step):
        pairs = [
            (h * low + l, ((h + step) % high) * low + l) for h in range(high) for l in range(low)
        ]
        return lax.ppermute(value, "sp", pairs)

    def over_low(value):
        return lax.ppermute(value, "sp", [(i, i ^ 1) for i in range(sp)])

    def over_wide(value):
        return lax.ppermute(value, "tp", [(i, (i + core) % tp) for i in range(tp)])

    def over_core(value):
        return lax.ppermute(value, "tp", [(i, i ^ 1) for i in range(tp)])

    high_groups = [[h * low + l for h in range(high)] for l in range(low)]

    def spread(piece):
        half = piece.shape[0] // 2
        by_low = over_low(piece)
        by_wide = over_wide(piece)
        across = jnp.concatenate([over_wide(by_low[:half]), over_low(by_wide[half:])], axis=0)
        mine = [[piece, by_wide], [by_low, across]]
        return [[[one, over_core(one)] for one in row] for row in mine]

    def local(
        resid,
        query_a,
        key_a,
        value_a,
        query_b,
        key_b,
        value_b,
        gain_qa,
        gain_ka,
        gain_qb,
        gain_kb,
        w_out_a,
        w_out_b,
        norm_gain,
        w_up,
        w_down,
    ):
        count = query_a.shape[0]
        width_a = gain_qa.shape[0]
        width_b = gain_qb.shape[0]
        model = resid.shape[1]
        s_index = lax.axis_index("sp")
        t_index = lax.axis_index("tp")
        l_index = s_index % low
        c_index = t_index % core
        x_index = t_index // core
        places = s_index * count + jnp.arange(count, dtype=jnp.int32)

        keys_a = norm_rope(key_a, gain_ka, places).reshape(count, -1)
        keys_b = norm_rope(key_b, gain_kb, places).reshape(count, -1)
        packed = jnp.concatenate([keys_b, value_b, keys_a, value_a], axis=1)
        blocks = [packed] + [over_high(packed, d) for d in range(1, high)]
        blocks = blocks + [over_low(block) for block in blocks]
        every = jnp.concatenate(blocks, axis=0)
        n_b, n_a = keys_b.shape[1], keys_a.shape[1]
        all_kb = every[:, :n_b].reshape(-1, n_b // width_b, width_b)
        all_vb = every[:, n_b : 2 * n_b].reshape(-1, n_b // width_b, width_b)
        all_ka = every[:, 2 * n_b : 2 * n_b + n_a].reshape(-1, n_a // width_a, width_a)
        all_va = every[:, 2 * n_b + n_a :].reshape(-1, n_a // width_a, width_a)

        queries_a = norm_rope(query_a, gain_qa, places)
        queries_b = norm_rope(query_b, gain_qb, places)
        kv_a, kv_b = n_a // width_a, n_b // width_b
        queries_a = queries_a.reshape(count, kv_a, -1, width_a)
        queries_b = queries_b.reshape(count, kv_b, -1, width_b)
        attn_a = attend(queries_a, all_ka, all_va, width_a ** (-0.5))
        attn_b = attend(queries_b, all_kb, all_vb, width_b ** (-0.5))

        attn = jnp.concatenate([attn_a, attn_b], axis=1)
        rows = count // tp
        attn = attn.reshape(wide, core, rows, -1)
        kept = lax.dynamic_index_in_dim(attn, c_index, 1, keepdims=False)
        sent = lax.dynamic_index_in_dim(attn, 1 - c_index, 1, keepdims=False)
        kept = kept.reshape(wide * rows, -1)
        came = over_core(sent.reshape(wide * rows, -1))
        w_out = jnp.concatenate([w_out_a, w_out_b], axis=0)
        w_out_other = over_core(w_out)
        part = jnp.dot(kept, w_out, preferred_element_type=jnp.float32) + jnp.dot(
            came, w_out_other, preferred_element_type=jnp.float32
        )
        part = part.reshape(wide, rows, model)
        part_kept = lax.dynamic_index_in_dim(part, x_index, 0, keepdims=False)
        part_sent = lax.dynamic_index_in_dim(part, 1 - x_index, 0, keepdims=False)
        part_came = over_wide(part_sent.astype(jnp.bfloat16)).astype(jnp.float32)
        mid = (resid.astype(jnp.float32) + (part_kept + part_came)).astype(jnp.bfloat16)
        midf = mid.astype(jnp.float32)
        normed = (
            midf * lax.rsqrt(jnp.mean(midf * midf, axis=-1, keepdims=True) + EPS) * norm_gain
        ).astype(jnp.bfloat16)

        block = w_up.shape[0]
        split = normed.reshape(rows, high, low, block)
        own = lax.dynamic_index_in_dim(split, l_index, 2, keepdims=False)
        other = lax.dynamic_index_in_dim(split, 1 - l_index, 2, keepdims=False)
        normed = jnp.concatenate([own.reshape(rows, -1), other.reshape(rows, -1)], axis=1)
        gathered = jnp.concatenate(
            [normed] + [over_high(normed, d) for d in range(1, high)], axis=0
        )

        up_piece = lax.all_to_all(
            w_up, "sp", split_axis=1, concat_axis=0, tiled=True, axis_index_groups=high_groups
        )
        down_piece = lax.all_to_all(
            w_down, "sp", split_axis=0, concat_axis=1, tiled=True, axis_index_groups=high_groups
        )
        ups = spread(up_piece)
        downs = spread(down_piece)

        inner = up_piece.shape[0]
        outs = [0.0, 0.0]
        for x in range(wide):
            for c in range(core):
                pre = jnp.dot(
                    gathered[:, :inner], ups[0][x][c], preferred_element_type=jnp.float32
                ) + jnp.dot(gathered[:, inner:], ups[1][x][c], preferred_element_type=jnp.float32)
                hidden = jnp.square(jax.nn.relu(pre)).astype(jnp.bfloat16)
                for l in range(low):
                    outs[l] = outs[l] + jnp.dot(
                        hidden, downs[l][x][c], preferred_element_type=jnp.float32
                    )
        out = jnp.concatenate(outs, axis=1)
        mixed = out[:rows]
        for d in range(1, high):
            mixed = mixed + over_high(
                out[d * rows : (d + 1) * rows].astype(jnp.bfloat16), -d
            ).astype(jnp.float32)
        first, second = mixed[:, :inner], mixed[:, inner:]
        even = jnp.where(l_index == 0, first, second).reshape(rows, high, 1, block)
        odd = jnp.where(l_index == 0, second, first).reshape(rows, high, 1, block)
        mixed = jnp.concatenate([even, odd], axis=2).reshape(rows, model)
        return (midf + mixed).astype(jnp.bfloat16)

    return local


def solution(mesh):
    return jax.shard_map(
        make_local(mesh.shape["sp"], mesh.shape["tp"]),
        mesh=mesh,
        in_specs=(
            P(("sp", "tp"), None),
            P("sp", "tp"),
            P("sp", "tp"),
            P("sp", "tp"),
            P("sp", "tp"),
            P("sp", "tp"),
            P("sp", "tp"),
            P(),
            P(),
            P(),
            P(),
            P("tp", None),
            P("tp", None),
            P(),
            P("sp", "tp"),
            P("tp", "sp"),
        ),
        out_specs=P(("sp", "tp"), None),
        check_vma=False,
    )
```
